32 devices in a mesh: tp: 4 (over y, x), dp: 8 (over z, core).
Axes of the slice: x: 2, y: 2, z: 4, core: 2. Of those that a mesh axis runs over, the one named last changes fastest.
Arguments:
- tokens: bfloat16 [128, 4096], P(None, 'dp'), may hold values from -15 to 15, as said below
- norm_gain: float32 [2, 4096], P(None, 'dp'), may hold values from 0.1 to 1.9
- w_query: bfloat16 [2, 4096, 2048], P(None, 'dp', 'tp'), may hold values from -0.09375 to 0.09375
- w_forget: bfloat16 [2, 4096, 2048], P(None, 'dp', 'tp'), may hold values from -0.09375 to 0.09375
- w_value: bfloat16 [2, 4096, 2048], P(None, 'dp', 'tp'), may hold values from -0.09375 to 0.09375
- w_gate: bfloat16 [2, 4096, 2048], P(None, 'dp', 'tp'), may hold values from -0.09375 to 0.09375
- floor_rate: float32 [2, 2048], P(None, 'tp'), may hold values from 0 to 0.9
- head_gain: float32 [2, 128], replicated, may hold values from 0.1 to 1.9
- w_output: bfloat16 [2, 2048, 4096], P(None, 'tp', 'dp'), may hold values from -0.3 to 0.3
- state: float32 [2, 128, 16, 128, 128], P(None, 'dp', 'tp'), may hold values from -4 to 4
Outputs:
- mixed: bfloat16 [128, 4096], P(None, 'dp')
- new_state: float32 [2, 128, 16, 128, 128], P(None, 'dp', 'tp')
The draws below stay inside these ranges and needn't reach their ends.
Inputs may be any that keep to these rules, and one draw needn't show every extreme that they name: `tokens`: activations whose feature blocks have different scales.
All inputs are finite; a program needn't handle non-finite values.
Results may differ from the reference program's by a relative error of at most 0.035.
Values may be sent and summed in bfloat16 or wider, within the bound.
A program may use at most 64 MiB of HBM per device.

```python
import jax
import jax.numpy as jnp
from jax import lax

D = 4096
H = 16
DK = 128
DV = 128
BATCH = 128
N_DP = 8


def draw_tokens(key, part):
    first, second, third = jax.random.split(key, 3)
    group_scales = jnp.exp(jax.random.uniform(second, (32,), jnp.float32, jnp.log(0.25), jnp.log(2.5)))
    column_scales = jnp.repeat(group_scales, D // 32)
    base = jnp.clip(jax.random.normal(first, (BATCH, D), jnp.float32), -5.9, 5.9)
    return (base * column_scales[None, :]).astype(jnp.bfloat16)


def draw_w_output(key, part):
    rows = H * DV
    keys = jax.random.split(jax.random.fold_in(key, 71), 5)
    even_signs = 2.0 * jax.random.randint(keys[0], (2, rows, 1), 0, 2).astype(jnp.float32) - 1.0
    odd_signs = 2.0 * jax.random.randint(keys[1], (2, rows, 1), 0, 2).astype(jnp.float32) - 1.0
    column_signs = 2.0 * jax.random.randint(keys[2], (2, 1, D), 0, 2).astype(jnp.float32) - 1.0
    block_parity = (jnp.arange(D) // (D // N_DP) % 2)[None, None, :]
    pattern = jnp.where(block_parity == 0, even_signs, odd_signs)
    sigma = 1.5 / jnp.sqrt(jnp.float32(rows))
    magnitude = jax.random.uniform(keys[3], (2, 1, D), jnp.float32, 0.02, 0.06)
    noise = jnp.clip(jax.random.normal(keys[4], (2, rows, D), jnp.float32), -5.0, 5.0) * sigma
    total = jnp.clip(pattern * column_signs * magnitude + noise, -0.298, 0.298)
    return total.astype(jnp.bfloat16)


def block_scale(own_key, extent, cuts, low, largest):
    gain = 1.0
    for dim, parts in cuts:
        heights = jax.random.uniform(jax.random.fold_in(jax.random.fold_in(own_key, 6), dim), (parts,), jnp.float32, low / len(cuts), largest / len(cuts))
        gain = gain * jnp.repeat(jnp.exp(heights), extent[dim] // parts).reshape((-1,) + (1,) * (len(extent) - 1 - dim))
    return gain


def normal_values(own_key, extent, spread, limit, cuts=(), held_as=jnp.bfloat16):
    level = block_scale(own_key, extent, cuts, -0.22, 0.18) if cuts else 1.0
    array = jax.random.normal(own_key, extent, jnp.float32) * spread * level
    return jnp.minimum(jnp.maximum(array, -limit), limit).astype(held_as)


def setup_inputs(seed: int = 0) -> dict:
    streams_of = jax.random.split(jax.random.key(seed), 11)
    return {
        "tokens": draw_tokens(jax.random.fold_in(streams_of[10], 71), 0),
        "norm_gain": jnp.clip(1.0 + 0.18 * jax.random.normal(streams_of[1], (2, D), jnp.float32), 0.1, 1.9),
        "w_query": normal_values(streams_of[2], (2, D, H * DK), D ** -0.5, 0.09375, ((1, 8), (2, 4))),
        "w_forget": normal_values(streams_of[3], (2, D, H * DK), D ** -0.5, 0.09375, ((1, 8), (2, 4))),
        "w_value": normal_values(streams_of[4], (2, D, H * DV), D ** -0.5, 0.09375, ((1, 8), (2, 4))),
        "w_gate": normal_values(streams_of[5], (2, D, H * DV), D ** -0.5, 0.09375, ((1, 8), (2, 4))),
        "floor_rate": jnp.clip(0.9 * jax.random.uniform(streams_of[6], (2, H * DK), jnp.float32) ** block_scale(streams_of[6], (2, H * DK), ((1, 4),), -0.2, 0.2), 0.0, 0.9),
        "head_gain": jnp.clip(1.0 + 0.18 * jax.random.normal(streams_of[7], (2, DV), jnp.float32), 0.1, 1.9),
        "w_output": draw_w_output(jax.random.fold_in(streams_of[10], 71), 0),
        "state": normal_values(streams_of[9], (2, BATCH, H, DK, DV), 0.5, 4.0, ((1, 8), (2, 4)), jnp.float32),
    }


EPS = 1e-06

def mixer_layer(tokens, norm_gain, w_query, w_forget, w_value, w_gate, floor_rate, head_gain, w_output, old_state):
    tok = tokens.astype(jnp.float32)
    row_scale = lax.rsqrt(lax.optimization_barrier(jnp.mean(tok * tok, axis=-1, keepdims=True)) + EPS)
    normed = (tok * norm_gain).astype(jnp.bfloat16)
    blocks = normed.reshape(BATCH, N_DP, D // N_DP).astype(jnp.float32)

    def project(weight):
        pieces = weight.reshape(N_DP, D // N_DP, weight.shape[1]).astype(jnp.float32)
        partial_terms = jnp.einsum('bnd,ndc->nbc', blocks, pieces)
        rounded = lax.optimization_barrier(partial_terms.astype(jnp.bfloat16))
        total = lax.optimization_barrier(jnp.sum(rounded.astype(jnp.float32), axis=0))
        stored = lax.optimization_barrier((row_scale * total).astype(jnp.bfloat16))
        return stored.astype(jnp.float32).reshape(BATCH, H, -1)
    query = jax.nn.silu(project(w_query)) * DK ** (-0.5)
    forget_pre = project(w_forget)
    value = project(w_value)
    gate_pre = project(w_gate)
    floor_heads = floor_rate.reshape(H, DK)
    forget = floor_heads + (1.0 - floor_heads) * jax.nn.sigmoid(forget_pre)
    key_in = (1.0 - floor_heads) * jax.nn.sigmoid(-forget_pre)
    updated = old_state * forget[..., None] + key_in[..., None] * value[:, :, None, :]
    read = jnp.einsum('bhk,bhkv->bhv', query, updated, precision=lax.Precision.HIGHEST)
    read = read * lax.rsqrt(lax.optimization_barrier(jnp.mean(read * read, axis=-1, keepdims=True)) + EPS) * head_gain
    gated = (read * jax.nn.silu(gate_pre)).reshape(BATCH, H * DV).astype(jnp.bfloat16)
    update = jnp.dot(gated, w_output, preferred_element_type=jnp.float32)
    return ((tok + update).astype(jnp.bfloat16), updated)

def reference(tokens, norm_gain, w_query, w_forget, w_value, w_gate, floor_rate, head_gain, w_output, state):
    current = tokens
    states = []
    for layer_index in range(2):
        current, updated = mixer_layer(current, norm_gain[layer_index], w_query[layer_index], w_forget[layer_index], w_value[layer_index], w_gate[layer_index], floor_rate[layer_index], head_gain[layer_index], w_output[layer_index], state[layer_index])
        states.append(updated)
    return (current, jnp.stack(states, axis=0))
```

```python
import functools

import jax
import jax.numpy as jnp
from jax import lax
from jax.experimental import pallas as pl
from jax.experimental.pallas import tpu as pltpu
from jax.sharding import PartitionSpec as P

EPS = 1e-06
MESH = pl.DeviceIdType.MESH
F32 = jnp.float32
BF16 = jnp.bfloat16


def kernel(
    cfg, tok_h, gain, wq_h, wf_h, wv_h, wg_h, floor, hgain, wo_h, st_h,
    mixed_h, new_h,
    cur, w, wo, st, sqs, sqr, part, arecv, psum, brecv, gall, opart, trecv,
    ld_tok, ld_w, ld_wo, ld_st, out_sem, mix_sem,
    sq_s, sq_r, a_s, a_r, b_s, b_r, g_s, g_r, t_s, t_r, u_s, u_r,
):
    layers, n, nt, rows, hd, dk, feat, batch = cfg
    nz = n // 2
    share = batch // nt
    width = hd * dk
    me = lax.axis_index("dp")
    mt = lax.axis_index("tp")
    zme, core = me // 2, lax.rem(me, 2)
    w_h = (wq_h, wf_h, wv_h, wg_h)

    tok_load = pltpu.make_async_copy(tok_h, cur.at[0], ld_tok)
    tok_load.start()
    w_loads = [
        [pltpu.make_async_copy(w_h[p].at[l], w.at[l, p], ld_w.at[l, p]) for p in range(4)]
        for l in range(layers)
    ]
    st_loads = [
        [pltpu.make_async_copy(st_h.at[l, :, h], st.at[l, :, h], ld_st.at[l, h]) for h in range(hd)]
        for l in range(layers)
    ]
    wo_loads = [pltpu.make_async_copy(wo_h.at[l], wo.at[l], ld_wo.at[l]) for l in range(layers)]
    for l in range(layers):
        for p in range(4):
            w_loads[l][p].start()
        for h in range(hd):
            st_loads[l][h].start()
        wo_loads[l].start()

    barrier = pltpu.get_barrier_semaphore()
    for j in range(1, n):
        pl.semaphore_signal(barrier, inc=1, device_id={"dp": lax.rem(me + j, n)}, device_id_type=MESH)
    for j in range(1, nt):
        pl.semaphore_signal(barrier, inc=1, device_id={"tp": lax.rem(mt + j, nt)}, device_id_type=MESH)

    def remote(src, dst, ssem, rsem, dev):
        return pltpu.make_async_remote_copy(
            src_ref=src, dst_ref=dst, send_sem=ssem, recv_sem=rsem, device_id=dev, device_id_type=MESH
        )

    def sq_copy(l, j):
        return remote(sqs.at[l], sqr.at[l, j - 1], sq_s.at[l, j - 1], sq_r.at[l, j - 1],
                      {"dp": lax.rem(me + j, n)})

    def a_copy(l, h):
        return remote(part.at[l, h, :, 1 - core], arecv.at[l, h], a_s.at[l, h], a_r.at[l, h],
                      {"dp": zme * 2 + (1 - core)})

    def b_copy(l, h, j):
        z = lax.rem(zme + j, nz)
        return remote(psum.at[l, h, z], brecv.at[l, h, j - 1], b_s.at[l, h, j - 1], b_r.at[l, h, j - 1],
                      {"dp": z * 2 + core})

    def g_copy(l, j):
        mine = pl.ds(pl.multiple_of(me * rows, rows), rows)
        return remote(gall.at[l, mine], gall.at[l, mine], g_s.at[l, j - 1], g_r.at[l, j - 1],
                      {"dp": lax.rem(me + j, n)})

    def t_copy(l, j):
        t = lax.rem(mt + j, nt)
        return remote(opart.at[l, pl.ds(pl.multiple_of(t * share, share), share)], trecv.at[l, j - 1],
                      t_s.at[l, j - 1], t_r.at[l, j - 1], {"tp": t})

    def u_copy(l, j):
        mine = pl.ds(pl.multiple_of(mt * share, share), share)
        return remote(cur.at[l + 1, mine], cur.at[l + 1, mine], u_s.at[l, j - 1], u_r.at[l, j - 1],
                      {"tp": lax.rem(mt + j, nt)})

    tok_load.wait()
    for l in range(layers):
        tok = cur[l].astype(F32)
        own_sq = jnp.sum(tok * tok, axis=1, keepdims=True)
        eye = lax.broadcasted_iota(jnp.int32, (batch, batch), 0) == lax.broadcasted_iota(
            jnp.int32, (batch, batch), 1)
        sq_row = jnp.sum(jnp.where(eye, own_sq, 0.0), axis=0, keepdims=True)
        sqs[l] = jnp.broadcast_to(sq_row, (8, batch))
        if l == 0:
            pl.semaphore_wait(barrier, n + nt - 2)
        for j in range(1, n):
            sq_copy(l, j).start()
        normed = (tok * gain[l : l + 1, :]).astype(BF16)
        for p in range(4):
            w_loads[l][p].wait()
        for h in range(hd):
            for p in range(4):
                prod = jnp.dot(normed, w[l, p, :, h * dk : (h + 1) * dk], preferred_element_type=F32)
                part[l, h, :, :, :, p * dk : (p + 1) * dk] = prod.astype(BF16).reshape(nz, 2, rows, dk)
            a_copy(l, h).start()

        def pair(h, _, l=l):
            a_copy(l, h).wait_recv()
            total = part[l, h, :, core].astype(F32) + arecv[l, h].astype(F32)
            psum[l, h] = total.astype(BF16)
            for j in range(1, nz):
                b_copy(l, h, j).start()
            return 0

        lax.fori_loop(0, hd, pair, 0)

        sq_all = sqs[l]
        for j in range(1, n):
            sq_copy(l, j).wait_recv()
            sq_all = sq_all + sqr[l, j - 1]
        pick = lax.broadcasted_iota(jnp.int32, (rows, batch), 1) == me * rows + lax.broadcasted_iota(
            jnp.int32, (rows, batch), 0)
        own = jnp.sum(jnp.where(pick, sq_all[0:1, :], 0.0), axis=1, keepdims=True)
        scale = lax.rsqrt(own / (feat * n) + EPS)
        hg = hgain[l : l + 1, :]

        def head(h, _, l=l, scale=scale, hg=hg):
            summed = psum[l, h, zme].astype(F32)
            for j in range(1, nz):
                b_copy(l, h, j).wait_recv()
                summed = summed + brecv[l, h, j - 1].astype(F32)
            stored = (scale * summed).astype(BF16).astype(F32)
            q_pre, f_pre = stored[:, :dk], stored[:, dk : 2 * dk]
            value, g_pre = stored[:, 2 * dk : 3 * dk], stored[:, 3 * dk :]
            query = q_pre * jax.nn.sigmoid(q_pre) * dk ** (-0.5)
            fl = floor[l, pl.ds(h, 1), :]
            forget = fl + (1.0 - fl) * jax.nn.sigmoid(f_pre)
            key_in = (1.0 - fl) * jax.nn.sigmoid(-f_pre)
            stack = [query, forget, key_in]
            pad = -(3 * rows) % 128
            if pad:
                stack.append(jnp.zeros((pad, dk), F32))
            cols = jnp.concatenate(stack, axis=0).T
            pltpu.make_async_copy(st_h.at[l, :, h], st.at[l, :, h], ld_st.at[l, h]).wait()
            reads = []
            for b in range(rows):
                updated = (
                    st[l, b, h] * cols[:, rows + b : rows + b + 1]
                    + cols[:, 2 * rows + b : 2 * rows + b + 1] * value[b : b + 1, :]
                )
                st[l, b, h] = updated
                reads.append(jnp.sum(cols[:, b : b + 1] * updated, axis=0, keepdims=True))
            pltpu.make_async_copy(st.at[l, :, h], new_h.at[l, :, h], out_sem.at[l, h]).start()
            read = jnp.concatenate(reads, axis=0)
            read = read * lax.rsqrt(jnp.mean(read * read, axis=-1, keepdims=True) + EPS) * hg
            gated = (read * (g_pre * jax.nn.sigmoid(g_pre))).astype(BF16)
            gall[l, pl.ds(pl.multiple_of(me * rows, rows), rows),
                 pl.ds(pl.multiple_of(h * dk, dk), dk)] = gated
            return 0

        lax.fori_loop(0, hd, head, 0)

        for j in range(1, n):
            g_copy(l, j).start()
        wo_loads[l].wait()
        for j in range(1, n):
            g_copy(l, j).wait_recv()
        update = jnp.dot(gall[l], wo[l], preferred_element_type=F32)
        opart[l] = update.astype(BF16)
        for j in range(1, nt):
            t_copy(l, j).start()
        mine = pl.ds(pl.multiple_of(mt * share, share), share)
        total = opart[l, mine, :].astype(F32)
        for j in range(1, nt):
            t_copy(l, j).wait_recv()
            total = total + trecv[l, j - 1].astype(F32)
        cur[l + 1, mine, :] = (cur[l, mine, :].astype(F32) + total).astype(BF16)
        for j in range(1, nt):
            u_copy(l, j).start()
        for j in range(1, nt):
            u_copy(l, j).wait_recv()

    mixed = pltpu.make_async_copy(cur.at[layers], mixed_h, mix_sem)
    mixed.start()
    for l in range(layers):
        for j in range(1, n):
            sq_copy(l, j).wait_send()
            g_copy(l, j).wait_send()
        for j in range(1, nt):
            t_copy(l, j).wait_send()
            u_copy(l, j).wait_send()

        def drain(h, _, l=l):
            a_copy(l, h).wait_send()
            for j in range(1, nz):
                b_copy(l, h, j).wait_send()
            pltpu.make_async_copy(st.at[l, :, h], new_h.at[l, :, h], out_sem.at[l, h]).wait()
            return 0

        lax.fori_loop(0, hd, drain, 0)
    mixed.wait()


def per_device(
    n, nt, tokens, norm_gain, w_query, w_forget, w_value, w_gate, floor_rate, head_gain, w_output, state
):
    layers, rows, hd, dk, _ = state.shape
    batch, feat = tokens.shape
    width = hd * dk
    nz = n // 2
    share = batch // nt
    cfg = (layers, n, nt, rows, hd, dk, feat, batch)
    dma = pltpu.SemaphoreType.DMA
    vmem = pl.BlockSpec(memory_space=pltpu.VMEM)
    hbm = pl.BlockSpec(memory_space=pl.ANY)
    mixed, new_state = pl.pallas_call(
        functools.partial(kernel, cfg),
        out_shape=(
            jax.ShapeDtypeStruct(tokens.shape, BF16),
            jax.ShapeDtypeStruct(state.shape, F32),
        ),
        in_specs=[hbm, vmem, hbm, hbm, hbm, hbm, vmem, vmem, hbm, hbm],
        out_specs=(hbm, hbm),
        scratch_shapes=[
            pltpu.VMEM((layers + 1, batch, feat), BF16),
            pltpu.VMEM((layers, 4, feat, width), BF16),
            pltpu.VMEM((layers, width, feat), BF16),
            pltpu.VMEM(state.shape, F32),
            pltpu.VMEM((layers, 8, batch), F32),
            pltpu.VMEM((layers, n - 1, 8, batch), F32),
            pltpu.VMEM((layers, hd, nz, 2, rows, 4 * dk), BF16),
            pltpu.VMEM((layers, hd, nz, rows, 4 * dk), BF16),
            pltpu.VMEM((layers, hd, nz, rows, 4 * dk), BF16),
            pltpu.VMEM((layers, hd, nz - 1, rows, 4 * dk), BF16),
            pltpu.VMEM((layers, batch, width), BF16),
            pltpu.VMEM((layers, batch, feat), BF16),
            pltpu.VMEM((layers, nt - 1, share, feat), BF16),
            dma(()), dma((layers, 4)), dma((layers,)), dma((layers, hd)), dma((layers, hd)), dma(()),
            dma((layers, n - 1)), dma((layers, n - 1)),
            dma((layers, hd)), dma((layers, hd)),
            dma((layers, hd, nz - 1)), dma((layers, hd, nz - 1)),
            dma((layers, n - 1)), dma((layers, n - 1)),
            dma((layers, nt - 1)), dma((layers, nt - 1)),
            dma((layers, nt - 1)), dma((layers, nt - 1)),
        ],
        compiler_params=pltpu.CompilerParams(
            collective_id=0, has_side_effects=True, vmem_limit_bytes=48 * 1024 * 1024
        ),
    )(
        tokens, norm_gain, w_query, w_forget, w_value, w_gate,
        floor_rate.reshape(layers, hd, dk), head_gain, w_output, state,
    )
    return mixed, new_state


def solution(mesh):
    in_specs = (
        P(None, "dp"),
        P(None, "dp"),
        P(None, "dp", "tp"),
        P(None, "dp", "tp"),
        P(None, "dp", "tp"),
        P(None, "dp", "tp"),
        P(None, "tp"),
        P(),
        P(None, "tp", "dp"),
        P(None, "dp", "tp", None, None),
    )
    out_specs = (P(None, "dp"), P(None, "dp", "tp", None, None))
    return jax.shard_map(
        functools.partial(per_device, mesh.shape["dp"], mesh.shape["tp"]),
        mesh=mesh, in_specs=in_specs, out_specs=out_specs, check_vma=False,
    )
```

```python
import functools

import jax
import jax.numpy as jnp
from jax import lax
from jax.experimental import pallas as pl
from jax.experimental.pallas import tpu as pltpu
from jax.sharding import PartitionSpec as P

EPS = 1e-06
MESH = pl.DeviceIdType.MESH
F32 = jnp.float32
BF16 = jnp.bfloat16


def kernel(
    cfg, tok_h, gain_h, wq_h, wf_h, wv_h, wg_h, floor_h, hgain_h, wo_h, st_h,
    mixed, st,
    cur, gain, floor, hgain, w, wo, colbuf, valbuf, sqs, sqr, part, arecv, psum, brecv, gall, opart, trecv,
    ld_tok, ld_w, ld_wo, ld_st, ld_small,
    sq_s, sq_r, a_s, a_r, b_s, b_r, g_s, g_r, t_s, t_r, u_s, u_r,
):
    layers, n, nt, rows, hd, dk, feat, batch, nc = cfg
    part_feat = feat // nc
    nz = n // 2
    share = batch // nt
    width = hd * dk
    me = lax.axis_index("dp")
    mt = lax.axis_index("tp")
    zme, core = me // 2, lax.rem(me, 2)
    w_h = (wq_h, wf_h, wv_h, wg_h)

    tok_loads = [
        pltpu.make_async_copy(tok_h.at[:, pl.ds(c * part_feat, part_feat)], cur.at[0, c], ld_tok.at[c])
        for c in range(nc)
    ]
    small = [
        pltpu.make_async_copy(src, dst, ld_small.at[i])
        for i, (src, dst) in enumerate(((gain_h, gain), (floor_h, floor), (hgain_h, hgain)))
    ]
    for load in tok_loads + small:
        load.start()
    w_loads = [
        [pltpu.make_async_copy(w_h[p].at[l], w.at[l, p], ld_w.at[l, p]) for p in range(4)]
        for l in range(layers)
    ]
    st_loads = [
        [pltpu.make_async_copy(st_h.at[l, :, h], st.at[l, :, h], ld_st.at[l, h]) for h in range(hd)]
        for l in range(layers)
    ]
    wo_loads = [pltpu.make_async_copy(wo_h.at[l], wo.at[l], ld_wo.at[l]) for l in range(layers)]
    for load in w_loads[0]:
        load.start()

    barrier = pltpu.get_barrier_semaphore()
    for j in range(1, n):
        pl.semaphore_signal(barrier, inc=1, device_id={"dp": lax.rem(me + j, n)}, device_id_type=MESH)
    for j in range(1, nt):
        pl.semaphore_signal(barrier, inc=1, device_id={"tp": lax.rem(mt + j, nt)}, device_id_type=MESH)

    def remote(src, dst, ssem, rsem, dev):
        return pltpu.make_async_remote_copy(
            src_ref=src, dst_ref=dst, send_sem=ssem, recv_sem=rsem, device_id=dev, device_id_type=MESH
        )

    def whole(l):
        return jnp.concatenate([cur[l, c] for c in range(nc)], axis=1)

    def sq_copy(l, j):
        return remote(sqs.at[l], sqr.at[l, j - 1], sq_s.at[l, j - 1], sq_r.at[l, j - 1],
                      {"dp": lax.rem(me + j, n)})

    def a_copy(l, h):
        return remote(part.at[l, h, :, 1 - core], arecv.at[l, h], a_s.at[l, h], a_r.at[l, h],
                      {"dp": zme * 2 + (1 - core)})

    def b_copy(l, h, j):
        z = lax.rem(zme + j, nz)
        return remote(psum.at[l, h, z], brecv.at[l, h, j - 1], b_s.at[l, h, j - 1], b_r.at[l, h, j - 1],
                      {"dp": z * 2 + core})

    def g_copy(l, h, j):
        mine = pl.ds(pl.multiple_of(me * rows, rows), rows)
        return remote(gall.at[l, h, mine], gall.at[l, h, mine], g_s.at[l, h, j - 1], g_r.at[l, h, j - 1],
                      {"dp": lax.rem(me + j, n)})

    def t_copy(l, c, j):
        t = lax.rem(mt + j, nt)
        return remote(opart.at[l, c, pl.ds(pl.multiple_of(t * share, share), share)], trecv.at[l, c, j - 1],
                      t_s.at[l, c, j - 1], t_r.at[l, c, j - 1], {"tp": t})

    def u_copy(l, c, j):
        mine = pl.ds(pl.multiple_of(mt * share, share), share)
        return remote(cur.at[l + 1, c, mine], cur.at[l + 1, c, mine], u_s.at[l, c, j - 1], u_r.at[l, c, j - 1],
                      {"tp": lax.rem(mt + j, nt)})

    for load in tok_loads + small:
        load.wait()
    for l in range(layers):
        tok = whole(l).astype(F32)
        own_sq = jnp.sum(tok * tok, axis=1, keepdims=True)
        eye = lax.broadcasted_iota(jnp.int32, (batch, batch), 0) == lax.broadcasted_iota(
            jnp.int32, (batch, batch), 1)
        sq_row = jnp.sum(jnp.where(eye, own_sq, 0.0), axis=0, keepdims=True)
        sqs[l] = jnp.broadcast_to(sq_row, (8, batch))
        if l == 0:
            pl.semaphore_wait(barrier, n + nt - 2)
        for j in range(1, n):
            sq_copy(l, j).start()
        normed = (tok * gain[l : l + 1, :]).astype(BF16)
        for p in range(4):
            w_loads[l][p].wait()
        if l == 0:
            for load in st_loads[0] + [wo_loads[0]]:
                load.start()
        for h in range(hd):
            for p in range(4):
                prod = jnp.dot(normed, w[l, p, :, h * dk : (h + 1) * dk], preferred_element_type=F32)
                part[l, h, :, :, :, p * dk : (p + 1) * dk] = prod.astype(BF16).reshape(nz, 2, rows, dk)
            a_copy(l, h).start()

        def pair(h, _, l=l):
            a_copy(l, h).wait_recv()
            total = part[l, h, :, core].astype(F32) + arecv[l, h].astype(F32)
            psum[l, h] = total.astype(BF16)
            for j in range(1, nz):
                b_copy(l, h, j).start()
            return 0

        lax.fori_loop(0, hd, pair, 0)

        sq_all = sqs[l]
        for j in range(1, n):
            sq_copy(l, j).wait_recv()
            sq_all = sq_all + sqr[l, j - 1]
        pick = lax.broadcasted_iota(jnp.int32, (rows, batch), 1) == me * rows + lax.broadcasted_iota(
            jnp.int32, (rows, batch), 0)
        own = jnp.sum(jnp.where(pick, sq_all[0:1, :], 0.0), axis=1, keepdims=True)
        scale = lax.rsqrt(own / (feat * n) + EPS)
        hg = hgain[l : l + 1, :]

        def head(h, _, l=l, scale=scale, hg=hg):
            summed = psum[l, h, zme].astype(F32)
            for j in range(1, nz):
                b_copy(l, h, j).wait_recv()
                summed = summed + brecv[l, h, j - 1].astype(F32)
            stored = (scale * summed).astype(BF16).astype(F32)
            q_pre, f_pre = stored[:, :dk], stored[:, dk : 2 * dk]
            value, g_pre = stored[:, 2 * dk : 3 * dk], stored[:, 3 * dk :]
            query = q_pre * jax.nn.sigmoid(q_pre) * dk ** (-0.5)
            fl = floor[l : l + 1, pl.ds(pl.multiple_of(h * dk, dk), dk)]
            forget = fl + (1.0 - fl) * jax.nn.sigmoid(f_pre)
            key_in = (1.0 - fl) * jax.nn.sigmoid(-f_pre)
            stack = [query * forget, forget, key_in]
            pad = -(3 * rows) % 128
            if pad:
                stack.append(jnp.zeros((pad, dk), F32))
            cols = jnp.concatenate(stack, axis=0).T
            pltpu.make_async_copy(st_h.at[l, :, h], st.at[l, :, h], ld_st.at[l, h]).wait()
            colbuf[h] = cols
            valbuf[h] = value
            reads = [
                jnp.sum(cols[:, b : b + 1] * st[l, b, h], axis=0, keepdims=True) for b in range(rows)
            ]
            along = jnp.sum(query * key_in, axis=-1, keepdims=True)
            read = jnp.concatenate(reads, axis=0) + along * value
            read = read * lax.rsqrt(jnp.mean(read * read, axis=-1, keepdims=True) + EPS) * hg
            gated = (read * (g_pre * jax.nn.sigmoid(g_pre))).astype(BF16)
            gall[l, h, pl.ds(pl.multiple_of(me * rows, rows), rows), :] = gated
            for j in range(1, n):
                g_copy(l, h, j).start()
            return 0

        lax.fori_loop(0, hd, head, 0)

        if l + 1 < layers:
            for load in w_loads[l + 1] + st_loads[l + 1] + [wo_loads[l + 1]]:
                load.start()

        def renew(h, _, l=l):
            cols, value = colbuf[h], valbuf[h]
            for b in range(rows):
                st[l, b, h] = (
                    st[l, b, h] * cols[:, rows + b : rows + b + 1]
                    + cols[:, 2 * rows + b : 2 * rows + b + 1] * value[b : b + 1, :]
                )
            return 0

        lax.fori_loop(0, hd, renew, 0)

        wo_loads[l].wait()
        for h in range(hd):
            for j in range(1, n):
                g_copy(l, h, j).wait_recv()
        gathered = jnp.concatenate([gall[l, h] for h in range(hd)], axis=1)
        for c in range(nc):
            cols = slice(c * part_feat, (c + 1) * part_feat)
            update = jnp.dot(gathered, wo[l, :, cols], preferred_element_type=F32)
            opart[l, c] = update.astype(BF16)
            for j in range(1, nt):
                t_copy(l, c, j).start()
        mine = pl.ds(pl.multiple_of(mt * share, share), share)
        for c in range(nc):
            cols = slice(c * part_feat, (c + 1) * part_feat)
            total = opart[l, c, mine, :].astype(F32)
            for j in range(1, nt):
                t_copy(l, c, j).wait_recv()
                total = total + trecv[l, c, j - 1].astype(F32)
            cur[l + 1, c, mine, :] = (cur[l, c, mine, :].astype(F32) + total).astype(BF16)
            for j in range(1, nt):
                u_copy(l, c, j).start()
        for c in range(nc):
            for j in range(1, nt):
                u_copy(l, c, j).wait_recv()

    mixed[...] = whole(layers)
    for l in range(layers):
        for j in range(1, n):
            sq_copy(l, j).wait_send()
        for c in range(nc):
            for j in range(1, nt):
                t_copy(l, c, j).wait_send()
                u_copy(l, c, j).wait_send()

        def drain(h, _, l=l):
            a_copy(l, h).wait_send()
            for j in range(1, nz):
                b_copy(l, h, j).wait_send()
            for j in range(1, n):
                g_copy(l, h, j).wait_send()
            return 0

        lax.fori_loop(0, hd, drain, 0)


def flush(mixed, st, mixed_h, new_h, st_sem, mix_sem):
    copies = [
        pltpu.make_async_copy(st.at[l, :, h], new_h.at[l, :, h], st_sem.at[l, h])
        for l in range(st.shape[0])
        for h in range(st.shape[2])
    ]
    copies.append(pltpu.make_async_copy(mixed, mixed_h, mix_sem))
    for copy in copies:
        copy.start()
    for copy in copies:
        copy.wait()


def per_device(
    n, nt, tokens, norm_gain, w_query, w_forget, w_value, w_gate, floor_rate, head_gain, w_output, state
):
    layers, rows, hd, dk, _ = state.shape
    batch, feat = tokens.shape
    width = hd * dk
    nz = n // 2
    share = batch // nt
    nc = 2
    cfg = (layers, n, nt, rows, hd, dk, feat, batch, nc)
    dma = pltpu.SemaphoreType.DMA
    vmem = pl.BlockSpec(memory_space=pltpu.VMEM)
    hbm_or_vmem = pl.BlockSpec(memory_space=pl.ANY)
    hbm = pl.BlockSpec(memory_space=pltpu.HBM)
    mixed, new_state = pl.pallas_call(
        functools.partial(kernel, cfg),
        out_shape=(
            jax.ShapeDtypeStruct(tokens.shape, BF16),
            jax.ShapeDtypeStruct(state.shape, F32),
        ),
        in_specs=[hbm] * 10,
        out_specs=(vmem, vmem),
        scratch_shapes=[
            pltpu.VMEM((layers + 1, nc, batch, feat // nc), BF16),
            pltpu.VMEM(norm_gain.shape, F32),
            pltpu.VMEM(floor_rate.shape, F32),
            pltpu.VMEM(head_gain.shape, F32),
            pltpu.VMEM((layers, 4, feat, width), BF16),
            pltpu.VMEM((layers, width, feat), BF16),
            pltpu.VMEM((hd, dk, -(-3 * rows // 128) * 128), F32),
            pltpu.VMEM((hd, rows, dk), F32),
            pltpu.VMEM((layers, 8, batch), F32),
            pltpu.VMEM((layers, n - 1, 8, batch), F32),
            pltpu.VMEM((layers, hd, nz, 2, rows, 4 * dk), BF16),
            pltpu.VMEM((layers, hd, nz, rows, 4 * dk), BF16),
            pltpu.VMEM((layers, hd, nz, rows, 4 * dk), BF16),
            pltpu.VMEM((layers, hd, nz - 1, rows, 4 * dk), BF16),
            pltpu.VMEM((layers, hd, batch, dk), BF16),
            pltpu.VMEM((layers, nc, batch, feat // nc), BF16),
            pltpu.VMEM((layers, nc, nt - 1, share, feat // nc), BF16),
            dma((nc,)), dma((layers, 4)), dma((layers,)), dma((layers, hd)), dma((3,)),
            dma((layers, n - 1)), dma((layers, n - 1)),
            dma((layers, hd)), dma((layers, hd)),
            dma((layers, hd, nz - 1)), dma((layers, hd, nz - 1)),
            dma((layers, hd, n - 1)), dma((layers, hd, n - 1)),
            dma((layers, nc, nt - 1)), dma((layers, nc, nt - 1)),
            dma((layers, nc, nt - 1)), dma((layers, nc, nt - 1)),
        ],
        compiler_params=pltpu.CompilerParams(
            collective_id=0, has_side_effects=True, vmem_limit_bytes=36 * 1024 * 1024
        ),
    )(
        *(
            pltpu.with_memory_space_constraint(array, pltpu.HBM)
            for array in (
                tokens, norm_gain, w_query, w_forget, w_value, w_gate,
                floor_rate, head_gain, w_output, state,
            )
        )
    )
    return pl.pallas_call(
        flush,
        out_shape=(
            jax.ShapeDtypeStruct(tokens.shape, BF16),
            jax.ShapeDtypeStruct(state.shape, F32),
        ),
        in_specs=[hbm_or_vmem, hbm_or_vmem],
        out_specs=(hbm, hbm),
        scratch_shapes=[dma((layers, hd)), dma(())],
        compiler_params=pltpu.CompilerParams(vmem_limit_bytes=1024 * 1024),
    )(mixed, new_state)


def solution(mesh):
    in_specs = (
        P(None, "dp"),
        P(None, "dp"),
        P(None, "dp", "tp"),
        P(None, "dp", "tp"),
        P(None, "dp", "tp"),
        P(None, "dp", "tp"),
        P(None, "tp"),
        P(),
        P(None, "tp", "dp"),
        P(None, "dp", "tp", None, None),
    )
    out_specs = (P(None, "dp"), P(None, "dp", "tp", None, None))
    return jax.shard_map(
        functools.partial(per_device, mesh.shape["dp"], mesh.shape["tp"]),
        mesh=mesh, in_specs=in_specs, out_specs=out_specs, check_vma=False,
    )
```
